512 devices in a mesh: gr: 2 (over z_hi), fs: 32 (over z_lo, y), tp: 8 (over x, core).
Axes of the slice: x: 4, y: 8, z: 8 (z_hi: 2, z_lo: 4; z = z_hi * 4 + z_lo), core: 2. Of those that a mesh axis runs over, the one named last changes fastest.
Arguments:
- tokens: bfloat16 [16384, 2048], P(('gr', 'fs')), may hold values from -6 to 6
- norm_gain: float32 [2048], P(('gr', 'fs')), may hold values from 0.1 to 1.9
- gate_train: float32 [32, 2048, 1024], P(None, ('gr', 'fs'), 'tp'), may hold values from -0.125 to 0.125
- up_train: float32 [32, 2048, 1024], P(None, ('gr', 'fs'), 'tp'), may hold values from -0.125 to 0.125
- down_train: float32 [32, 1024, 2048], P(None, 'tp', ('gr', 'fs')), may hold values from -0.1875 to 0.1875
- expert_ids: int32 [16384, 2], P(('gr', 'fs')), may hold values from 0 to 31, all different within a row; in each aligned block of 256 rows (0 to 255, 256 to 511, ...) at most 32 rows name the same one
- route_score: float32 [16384, 2], P(('gr', 'fs')), may hold values from 0.05 to 1
Outputs:
- gate_ready: bfloat16 [32, 2048, 1024], P('fs', None, 'tp')
- up_ready: bfloat16 [32, 2048, 1024], P('fs', None, 'tp')
- down_ready: bfloat16 [32, 1024, 2048], P('fs', 'tp')
- mixed: bfloat16 [16384, 2048], P(('gr', 'fs'), 'tp')
The draws below stay inside these ranges and needn't reach their ends.
Inputs may be any that keep to these rules, and one draw needn't show every extreme that they name: `expert_ids`: each row names two different experts. Among the 256 rows of one device no expert is named more than 32 times, and in every draw some expert is named exactly 32 times by some device's rows.
All inputs are finite; a program needn't handle non-finite values.
Results may differ from the reference program's by a relative error of at most 0.015.
Values may be sent and summed in bfloat16 or wider, within the bound.
A program may use at most 64 MiB of HBM per device.

```python
import math
import jax
import jax.numpy as jnp
import numpy as np
from jax import lax

D = 2048
FF = 1024
TOK_DEV = 256
EXPERTS = 32
CAP = 32
TOKENS = 16384
N_GR = 2
N_FS = 32
N_TP = 8


def block_levels(stream_key, dims, pieces, least, top_value):
    loudness, own = 1.0, jax.random.fold_in(stream_key, 6)
    for dim, parts in pieces:
        draws = jnp.exp(jax.random.uniform(jax.random.fold_in(own, dim), (parts,), jnp.float32, least / len(pieces), top_value / len(pieces)))
        loudness = loudness * jnp.repeat(draws, dims[dim] // parts).reshape([-1 if axis == dim else 1 for axis in range(len(dims))])
    return loudness


def assign_block(own_key, own, number, rows, count, top, most, slope):
    ranking = jax.random.permutation(own_key, count)
    crowded, usual = portions_of(count, rows * top, most, slope, True), portions_of(count, rows * top, most, slope, False)
    places = jnp.arange(count)

    def named(lengths, rotation):
        used = int((lengths > 0).sum())
        fixed = max(1, used // 4)
        moved = fixed + (places - fixed + rotation * (used - fixed)) % max(1, count - fixed)
        return jnp.zeros((count,), jnp.int32).at[ranking[jnp.where(places < fixed, places, moved)]].set(jnp.asarray(lengths, jnp.int32))

    lengths = jnp.where(number % 4 == 0, named(crowded, number // 4), named(usual, number - number // 4 - 1))
    mixed = jax.random.permutation(jax.random.fold_in(own, 3), count)
    source_of, receiver = mixed[0:count // 2 * 2:2], mixed[1:count // 2 * 2:2]
    slack = jnp.minimum(lengths[source_of] - 1, most - lengths[receiver]) // 2
    slack = jnp.where((source_of == ranking[0]) | (receiver == ranking[0]) | (lengths[receiver] == 0), 0, jnp.maximum(slack, 0))
    moved = jax.random.randint(jax.random.fold_in(own, 4), (count // 2,), 0, 1 << 20) % (slack + 1)
    lengths = lengths.at[source_of].add(-moved).at[receiver].add(moved)
    members = jnp.searchsorted(jnp.cumsum(lengths), jnp.arange(rows * top), side="right").astype(jnp.int32)
    table = members.reshape(top, rows).T
    table = table[jax.random.permutation(jax.random.fold_in(own, 1), rows)]
    rotation = jax.random.randint(jax.random.fold_in(own, 2), (rows, 1), 0, top)
    return jnp.take_along_axis(table, (jnp.arange(top)[None, :] + rotation) % top, axis=1)


def portions_of(amount, total, reach, slope, full):
    portions = [(1 << 20) // math.isqrt(standing ** slope) + 1 for standing in range(1, amount + 1)]
    largest = reach if full else min(reach, max(-(-total // amount), total * portions[0] // sum(portions)))
    least = 1 if total - largest >= amount - 1 else 0
    holding, rest = [largest] + [least] * (amount - 1), total - largest - least * (amount - 1)
    while rest > 0:
        candidates = [i for i in range(1, amount) if holding[i] < largest] or [i for i in range(1, amount) if holding[i] < reach]
        pool, left = sum([portions[i] for i in candidates]), rest
        for i in candidates:
            addition = min(reach - holding[i], max(1, left * portions[i] // pool), rest)
            holding[i] = holding[i] + addition
            rest = rest - addition
    return np.array(holding)


def gaussian(own_key, shape, scale, bound, split=(), kind=jnp.bfloat16):
    result = scale * jax.random.normal(own_key, shape, jnp.float32)
    if split:
        result = result * block_levels(own_key, shape, split, -0.22, 0.18)
    return jnp.clip(result, -bound, bound).astype(kind)


def setup_inputs(seed: int = 0) -> dict:
    key_list = jax.random.split(jax.random.key(seed), 8)
    tokens = gaussian(key_list[0], (TOKENS, D), 1.0, 6.0, ((0, 64),))
    norm_gain = jnp.clip(1.0 + 0.18 * jax.random.normal(key_list[1], (D,), jnp.float32), 0.1, 1.9)
    gate_train = gaussian(key_list[2], (EXPERTS, D, FF), D ** -0.5, 0.125, ((1, 64), (2, 8)), jnp.float32)
    up_train = gaussian(key_list[3], (EXPERTS, D, FF), D ** -0.5, 0.125, ((1, 64), (2, 8)), jnp.float32)
    down_train = gaussian(key_list[4], (EXPERTS, FF, D), FF ** -0.5, 0.1875, ((1, 8), (2, 64)), jnp.float32)
    expert_ids_keys = jax.random.split(jax.random.fold_in(key_list[5], 1), TOKENS // TOK_DEV)
    expert_ids_turns = jax.random.permutation(jax.random.fold_in(key_list[5], 3), TOKENS // TOK_DEV)
    expert_ids = jax.vmap(lambda own, number: assign_block(jax.random.fold_in(key_list[5], 2), own, number, TOK_DEV, EXPERTS, 2, CAP, 2))(expert_ids_keys, expert_ids_turns).reshape((TOKENS, 2))
    route_score = jnp.clip(jnp.exp(math.log(1.0) - 2.9957323 * jax.random.uniform(key_list[6], (TOKENS, 2), jnp.float32) ** block_levels(key_list[6], (TOKENS, 2), ((0, 64),), -0.2, 0.2)), 0.05, 1.0)
    return dict(tokens=tokens, norm_gain=norm_gain, gate_train=gate_train, up_train=up_train, down_train=down_train, expert_ids=expert_ids, route_score=route_score)


epsilon = 1e-06

def reference(tokens, norm_gain, gate_train, up_train, down_train, expert_ids, route_score):
    gate_ready = (norm_gain[None, :, None] * gate_train).astype(jnp.bfloat16)
    up_ready = (norm_gain[None, :, None] * up_train).astype(jnp.bfloat16)
    down_ready = down_train.astype(jnp.bfloat16)
    floated = tokens.astype(jnp.float32)
    normed = (floated * lax.rsqrt(lax.optimization_barrier(jnp.mean(floated * floated, axis=-1, keepdims=True)) + epsilon)).astype(jnp.bfloat16)
    route_share = route_score / lax.optimization_barrier(jnp.sum(route_score, axis=-1, keepdims=True))
    blocks = N_GR * N_FS
    picks = TOK_DEV * 2
    flat_ids = expert_ids.reshape(blocks, picks)
    flat_share = route_share.reshape(blocks, picks)
    token_of = ((jnp.arange(picks, dtype=jnp.int32) // 2)[None, :] + (jnp.arange(blocks, dtype=jnp.int32) * TOK_DEV)[:, None]).astype(jnp.int32)
    block_rows = jnp.broadcast_to(jnp.arange(blocks, dtype=jnp.int32)[:, None], (blocks, picks))
    hidden_block = FF // N_TP

    def per_expert(total, expert):
        matches = (flat_ids == expert).astype(jnp.int32)
        ranked = jnp.cumsum(matches, axis=1) - 1
        column = jnp.where(matches > 0, ranked, CAP).astype(jnp.int32)
        token_table = jnp.zeros((blocks, CAP), jnp.int32).at[block_rows, column].set(token_of, mode='drop')
        share_table = jnp.zeros((blocks, CAP), jnp.float32).at[block_rows, column].set(flat_share, mode='drop')
        token_index = token_table.reshape(-1)
        picked_rows = normed[token_index]
        gate_act = jnp.dot(picked_rows, gate_ready[expert], preferred_element_type=jnp.float32)
        up_act = jnp.dot(picked_rows, up_ready[expert], preferred_element_type=jnp.float32)
        hidden = (jax.nn.silu(gate_act) * up_act).astype(jnp.bfloat16)
        partial_value = jnp.einsum('rnh,nhk->rnk', hidden.reshape(-1, N_TP, hidden_block).astype(jnp.float32), down_ready[expert].reshape(N_TP, hidden_block, D).astype(jnp.float32))
        rounded = lax.optimization_barrier(partial_value.astype(jnp.bfloat16))
        expert_out = lax.optimization_barrier(jnp.sum(rounded.astype(jnp.float32), axis=1)).astype(jnp.bfloat16)
        total = total.at[token_index].add(share_table.reshape(-1)[:, None] * expert_out.astype(jnp.float32))
        return (total, None)
    start = jnp.zeros((TOKENS, D), jnp.float32)
    summed, _ = lax.scan(per_expert, start, jnp.arange(EXPERTS, dtype=jnp.int32))
    return (gate_ready, up_ready, down_ready, summed.astype(jnp.bfloat16))
```

```python
import jax
import jax.numpy as jnp
from jax import lax
from jax.experimental import pallas as pl
from jax.experimental.pallas import tpu as pltpu
from jax.sharding import PartitionSpec as P

EPS = 1e-06
NY, NZ, NX = 8, 4, 4
NF = NY * NZ
CAP = 32
MESH = pl.DeviceIdType.MESH
BF, F32 = jnp.bfloat16, jnp.float32


def ring_offset(j, n):
    return jnp.where(j % 2 == 1, (j + 1) // 2, n - j // 2)


def kernel(
    tok, ids_t, score, gain, gate, up, down,
    gate_o, up_o, down_o, mixed_o,
    wsend, wy, wz, tsend, xin, rt, p0, p1, own, psend, precv, sbuf, r1, r2, fin, ret,
    wy_r, wz_r, tk_r, g_r, s_r, ret_r, snd,
):
    g, f, t = lax.axis_index("gr"), lax.axis_index("fs"), lax.axis_index("tp")
    z, y, x, c = f // NY, f % NY, t // 2, t % 2
    zz = g * NZ + z
    right, left = ((x + 1) % NX) * 2 + c, ((x + 3) % NX) * 2 + c
    opp, part = ((x + 2) % NX) * 2 + c, x * 2 + (1 - c)

    def send(src, dst, ssem, rsem, dev):
        pltpu.make_async_remote_copy(
            src_ref=src, dst_ref=dst, send_sem=ssem, recv_sem=rsem,
            device_id=dev, device_id_type=MESH,
        ).start()

    def arrived(dst, rsem):
        pltpu.make_async_remote_copy(
            src_ref=dst, dst_ref=dst, send_sem=snd.at[0], recv_sem=rsem,
            device_id=(g, f, part), device_id_type=MESH,
        ).wait_recv()

    def sent(ref, ssem):
        pltpu.make_async_remote_copy(
            src_ref=ref, dst_ref=ref, send_sem=ssem, recv_sem=wy_r.at[0],
            device_id=(g, f, part), device_id_type=MESH,
        ).wait_send()

    def loop(lo, hi, fn):
        def body(i, carry):
            fn(i)
            return carry
        lax.fori_loop(lo, hi, body, 0)

    bar = pltpu.get_barrier_semaphore()

    def greet(dev):
        pl.semaphore_signal(bar, inc=1, device_id=dev, device_id_type=MESH)

    loop(1, NF, lambda i: greet((g, (f + i) % NF, t)))
    loop(0, NZ, lambda i: greet((1 - g, i * NY + y, t)))
    for tt in (right, left, part):
        greet((g, f, tt))

    def cast(e):
        yy, z2 = e % NY, e // NY
        wsend[yy, z2, 0:32, :] = (gain[...] * gate[e]).astype(BF)
        wsend[yy, z2, 32:64, :] = (gain[...] * up[e]).astype(BF)
        wsend[yy, z2, 64:96, :] = down[e].T.astype(BF)

    loop(0, NF, cast)
    pl.semaphore_wait(bar, NF - 1 + NZ + 3)

    def y_send(j):
        yy = (y + ring_offset(j, NY)) % NY
        send(wsend.at[yy], wy.at[y], snd.at[0], wy_r.at[y], (g, z * NY + yy, t))

    def z_send(block, s):
        row = zz * NY + s

        def one(j):
            to = (zz + ring_offset(j, 2 * NZ)) % (2 * NZ)
            send(block.at[to % NZ], wz.at[row], snd.at[1], wz_r.at[row],
                 (to // NZ, (to % NZ) * NY + y, t))

        loop(1, 2 * NZ, one)
        wz[row] = block[z]

    loop(1, NY, y_send)
    z_send(wsend.at[y], y)

    e_iota = lax.broadcasted_iota(jnp.int32, (NF, 256), 0)
    i0, i1 = ids_t[0:1, :], ids_t[1:2, :]
    hit = (i0 == e_iota) | (i1 == e_iota)
    before = (
        lax.broadcasted_iota(jnp.int32, (256, 256), 0)
        < lax.broadcasted_iota(jnp.int32, (256, 256), 1)
    )
    rank = jnp.dot(hit.astype(F32).astype(BF), before.astype(F32).astype(BF),
                   preferred_element_type=F32)
    rt[...] = jnp.where(hit, rank, -1.0)
    r_iota = lax.broadcasted_iota(jnp.int32, (CAP, 256), 0).astype(F32)

    def slots(e):
        mask = rt[pl.ds(e, 1), :] == r_iota
        p0[e] = jnp.where(mask & (ids_t[0:1, :] == e), 1.0, 0.0).astype(BF)
        p1[e] = jnp.where(mask & (ids_t[1:2, :] == e), 1.0, 0.0).astype(BF)

    loop(0, NF, slots)
    floated = tok[...].astype(F32)
    inv = lax.rsqrt(jnp.mean(floated * floated, axis=-1, keepdims=True) + EPS)
    cols = pl.ds(pl.multiple_of(t * 256, 256), 256)
    normed = (tok[:, cols].astype(F32) * inv).astype(BF)

    def gather_rows(b):
        e = pl.ds(b * 8, 8)
        pick = (p0[e] + p1[e]).reshape(256, 256)
        rows = jnp.dot(pick, normed, preferred_element_type=F32)
        tsend[e] = rows.astype(BF).reshape(8, CAP, 256)

    loop(0, NZ, gather_rows)

    def t_send(i):
        zt = (z + i // NY) % NZ
        e = zt * NY + (y + i % NY) % NY
        send(tsend.at[e], xin.at[t, f], snd.at[2], tk_r.at[f], (g, e, t))

    loop(1, NF, t_send)
    xin[t, f] = tsend[f]

    def y_forward(j):
        s = (y + NY - ring_offset(j, NY)) % NY
        arrived(wy.at[s], wy_r.at[s])
        z_send(wy.at[s], s)

    loop(1, NY, y_forward)

    def chunk(k):
        return (z + NZ - k) % NZ

    def x_first(k):
        q = chunk(k)

        def one(i):
            s = q * NY + i

            @pl.when(s != f)
            def _():
                arrived(xin.at[t, s], tk_r.at[s])

        loop(0, NY, one)
        blk = xin.at[t, pl.ds(q * NY, NY)]
        send(blk, blk, snd.at[3], g_r.at[0, k], (g, f, right))
        send(blk, blk, snd.at[3], g_r.at[1, k], (g, f, left))
        send(blk, blk, snd.at[3], g_r.at[4, k], (g, f, part))

    def x_second(k):
        q = chunk(k)
        for side, kind, to, lo in ((left, 0, right, 0), (right, 1, left, 4)):
            blk = xin.at[side, pl.ds(q * NY, NY)]
            half = xin.at[side, pl.ds(q * NY + lo, 4)]
            arrived(blk, g_r.at[kind, k])
            send(half, half, snd.at[3], g_r.at[kind + 2, k], (g, f, to))
            send(blk, blk, snd.at[3], g_r.at[kind + 5, k], (g, f, part))

    def x_third(k):
        q = chunk(k)
        arrived(xin.at[opp, pl.ds(q * NY, 4)], g_r.at[2, k])
        arrived(xin.at[opp, pl.ds(q * NY + 4, 4)], g_r.at[3, k])
        blk = xin.at[opp, pl.ds(q * NY, NY)]
        send(blk, blk, snd.at[3], g_r.at[7, k], (g, f, part))

    def x_step(k):
        @pl.when(k < NZ)
        def _():
            x_first(k)

        @pl.when((k >= 1) & (k < NZ + 1))
        def _():
            x_second(k - 1)

        @pl.when(k >= 2)
        def _():
            x_third(k - 2)

    loop(0, NZ + 2, x_step)
    flip = 1 - 2 * c

    def from_partner(k):
        q = pl.ds(chunk(k) * NY, NY)
        for side, kind in ((part, 4), (left + flip, 5), (right + flip, 6), (opp + flip, 7)):
            arrived(xin.at[side, q], g_r.at[kind, k])

    loop(0, NZ, from_partner)

    def w_arrived(i):
        @pl.when(i // NY != zz)
        def _():
            arrived(wz.at[i], wz_r.at[i])

    loop(0, 2 * NF, w_arrived)

    def layer(k):
        q = pl.ds(chunk(k) * NY, NY)
        acc = jnp.zeros((256, 256), F32)
        for s in range(8):
            w = jnp.concatenate(
                [wz[8 * s:8 * s + 8, 0:32, :].reshape(256, 128),
                 wz[8 * s:8 * s + 8, 32:64, :].reshape(256, 128)], axis=1)
            acc += jnp.dot(xin[s, q].reshape(256, 256), w, preferred_element_type=F32)
        a, b = acc[:, 0:128], acc[:, 128:256]
        hidden = (a / (1.0 + jnp.exp(-a)) * b).astype(BF)
        for j in range(NX):
            for cc in (1 - c, c):
                blk = ((x + j) % NX) * 2 + cc
                d = wz[pl.ds(blk * 8, 8), 64:96, :].reshape(256, 128)
                o = lax.dot_general(hidden, d, (((1,), (1,)), ((), ())),
                                    preferred_element_type=F32)
                if cc is c:
                    own[k, j] = o
                else:
                    psend[k, j] = o.astype(BF)
        send(psend.at[k], precv.at[k], snd.at[4], s_r.at[0, k], (g, f, part))

    def r_first(k):
        arrived(precv.at[k], s_r.at[0, k])
        sbuf[k, 1] = (own[k, 2] + precv[k, 2].astype(F32)).astype(BF)
        send(sbuf.at[k, 1, pl.ds(0, 128)], r1.at[k, 0], snd.at[5], s_r.at[1, k], (g, f, right))
        send(sbuf.at[k, 1, pl.ds(128, 128)], r1.at[k, 1], snd.at[5], s_r.at[2, k], (g, f, left))

    def r_second(k):
        lo, hi = pl.ds(0, 128), pl.ds(128, 128)
        arrived(r1.at[k, 0], s_r.at[1, k])
        sbuf[k, 0, lo] = (own[k, 1, lo] + precv[k, 1, lo].astype(F32) + r1[k, 0].astype(F32)).astype(BF)
        sbuf[k, 0, hi] = (own[k, 1, hi] + precv[k, 1, hi].astype(F32)).astype(BF)
        send(sbuf.at[k, 0], r2.at[k, 0], snd.at[6], s_r.at[3, k], (g, f, right))
        arrived(r1.at[k, 1], s_r.at[2, k])
        sbuf[k, 2, lo] = (own[k, 3, lo] + precv[k, 3, lo].astype(F32)).astype(BF)
        sbuf[k, 2, hi] = (own[k, 3, hi] + precv[k, 3, hi].astype(F32) + r1[k, 1].astype(F32)).astype(BF)
        send(sbuf.at[k, 2], r2.at[k, 1], snd.at[6], s_r.at[4, k], (g, f, left))

    def r_third(k):
        arrived(r2.at[k, 0], s_r.at[3, k])
        arrived(r2.at[k, 1], s_r.at[4, k])
        total = (own[k, 0] + precv[k, 0].astype(F32)) + r2[k, 0].astype(F32) + r2[k, 1].astype(F32)
        q = chunk(k)
        fin[q] = total.astype(BF).reshape(NY, CAP, 256)

        def back(i):
            s = q * NY + i

            @pl.when(s != f)
            def _():
                send(fin.at[q, i], ret.at[f], snd.at[7], ret_r.at[f], (g, s, t))

            @pl.when(s == f)
            def _():
                ret[s] = fin[q, i]

        loop(0, NY, back)

    def r_step(k):
        @pl.when(k < NZ)
        def _():
            layer(k)

        @pl.when((k >= 1) & (k < NZ + 1))
        def _():
            r_first(k - 1)

        @pl.when((k >= 2) & (k < NZ + 2))
        def _():
            r_second(k - 2)

        @pl.when(k >= 3)
        def _():
            r_third(k - 3)

    loop(0, NZ + 3, r_step)

    def store(i):
        rows = pl.ds(pl.multiple_of(i * 32, 32), 32)
        gate_o[0, rows, :] = wz[i, 0:32, :]
        up_o[0, rows, :] = wz[i, 32:64, :]

    loop(0, 2 * NF, store)
    for j in range(16):
        blk = wz[4 * j:4 * j + 4, 64:96, :].reshape(128, 128)
        down_o[0, :, 128 * j:128 * j + 128] = blk.astype(F32).T.astype(BF)

    def back_arrived(i):
        @pl.when(i != f)
        def _():
            arrived(ret.at[i], ret_r.at[i])

    loop(0, NF, back_arrived)
    rows = ret[...].reshape(NF * CAP, 256)
    dims = (((0,), (0,)), ((), ()))
    a = lax.dot_general(p0[...].reshape(NF * CAP, 256), rows, dims, preferred_element_type=F32)
    b = lax.dot_general(p1[...].reshape(NF * CAP, 256), rows, dims, preferred_element_type=F32)
    s0, s1 = score[:, 0:1], score[:, 1:2]
    both = s0 + s1
    mixed_o[...] = (a * (s0 / both) + b * (s1 / both)).astype(BF)

    sent(wsend.at[pl.ds(0, 7)], snd.at[0])
    sent(wz.at[pl.ds(0, 56)], snd.at[1])
    sent(tsend.at[pl.ds(0, NF - 1)], snd.at[2])
    sent(xin.at[pl.ds(0, 7)], snd.at[3])
    sent(psend, snd.at[4])
    sent(r1, snd.at[5])
    sent(r2, snd.at[6])
    sent(ret.at[pl.ds(0, NF - 1)], snd.at[7])


def on_device(tokens, norm_gain, gate_train, up_train, down_train, expert_ids, route_score):
    vm = pl.BlockSpec(memory_space=pltpu.VMEM)
    dma = pltpu.SemaphoreType.DMA
    sds = jax.ShapeDtypeStruct
    return tuple(pl.pallas_call(
        kernel,
        out_shape=(
            sds((1, 2048, 128), BF), sds((1, 2048, 128), BF), sds((1, 128, 2048), BF),
            sds((256, 256), BF),
        ),
        in_specs=[vm] * 7,
        out_specs=(vm,) * 4,
        scratch_shapes=[
            pltpu.VMEM((NY, NZ, 96, 128), BF),
            pltpu.VMEM((NY, NZ, 96, 128), BF),
            pltpu.VMEM((2 * NF, 96, 128), BF),
            pltpu.VMEM((NF, CAP, 256), BF),
            pltpu.VMEM((8, NF, CAP, 256), BF),
            pltpu.VMEM((NF, 256), F32),
            pltpu.VMEM((NF, CAP, 256), BF),
            pltpu.VMEM((NF, CAP, 256), BF),
            pltpu.VMEM((NZ, NX, 256, 256), F32),
            pltpu.VMEM((NZ, NX, 256, 256), BF),
            pltpu.VMEM((NZ, NX, 256, 256), BF),
            pltpu.VMEM((NZ, 3, 256, 256), BF),
            pltpu.VMEM((NZ, 2, 128, 256), BF),
            pltpu.VMEM((NZ, 2, 256, 256), BF),
            pltpu.VMEM((NZ, NY, CAP, 256), BF),
            pltpu.VMEM((NF, CAP, 256), BF),
            dma((NY,)), dma((2 * NF,)), dma((NF,)), dma((8, NZ)), dma((5, NZ)), dma((NF,)), dma((8,)),
        ],
        compiler_params=pltpu.CompilerParams(collective_id=0, has_side_effects=True),
    )(
        tokens, expert_ids.T, route_score, norm_gain[:, None], gate_train, up_train, down_train
    ))


def solution(mesh):
    return jax.shard_map(
        on_device,
        mesh=mesh,
        in_specs=(
            P(("gr", "fs"), None),
            P(("gr", "fs")),
            P(None, ("gr", "fs"), "tp"),
            P(None, ("gr", "fs"), "tp"),
            P(None, "tp", ("gr", "fs")),
            P(("gr", "fs"), None),
            P(("gr", "fs"), None),
        ),
        out_specs=(
            P("fs", None, "tp"),
            P("fs", None, "tp"),
            P("fs", "tp", None),
            P(("gr", "fs"), "tp"),
        ),
        check_vma=False,
    )
```

```python
import jax
import jax.numpy as jnp
from jax import lax
from jax.experimental import pallas as pl
from jax.experimental.pallas import tpu as pltpu
from jax.sharding import PartitionSpec as P

EPS = 1e-06
NY, NZ, NX = 8, 4, 4
NF = NY * NZ
NR = 2 * NZ
CAP = 32
CH, RB = 8, 128
LAG1, LAG2 = 2, 2
MESH = pl.DeviceIdType.MESH
BF, F32 = jnp.bfloat16, jnp.float32


def ring_offset(j, n):
    return jnp.where(j % 2 == 1, (j + 1) // 2, (n - j // 2) % n)


def loop(lo, hi, fn):
    def body(i, carry):
        fn(i)
        return carry

    lax.fori_loop(lo, hi, body, 0)


def column(row, n):
    eye = lax.broadcasted_iota(jnp.int32, (n, n), 0) == lax.broadcasted_iota(jnp.int32, (n, n), 1)
    return jnp.sum(jnp.where(eye, row, 0.0), axis=1, keepdims=True)


def kernel(
    tok, ids_t, score_t, gain_t, gate, up, down_t,
    gate_o, up_o, down_o, mixed_o,
    gain, wg, wd, wyg, wyd, zg, zd, tsend, xin, rt, p0, p1, hid,
    own, psend, precv, sbuf, r1, r2, fin, ret,
    yg_r, yd_r, zg_r, zd_r, tk_r, g_r, s_r, ret_r, snd,
):
    g, f, t = lax.axis_index("gr"), lax.axis_index("fs"), lax.axis_index("tp")
    z, y, x, c = f // NY, f % NY, t // 2, t % 2
    zz = g * NZ + z
    right, left = ((x + 1) % NX) * 2 + c, ((x + 3) % NX) * 2 + c
    opp, part = ((x + 2) % NX) * 2 + c, x * 2 + (1 - c)

    def send(src, dst, ssem, rsem, dev):
        pltpu.make_async_remote_copy(
            src_ref=src, dst_ref=dst, send_sem=ssem, recv_sem=rsem,
            device_id=dev, device_id_type=MESH,
        ).start()

    def arrived(dst, rsem):
        pltpu.make_async_remote_copy(
            src_ref=dst, dst_ref=dst, send_sem=snd.at[0], recv_sem=rsem,
            device_id=(g, f, part), device_id_type=MESH,
        ).wait_recv()

    def sent(ref, ssem):
        pltpu.make_async_remote_copy(
            src_ref=ref, dst_ref=ref, send_sem=ssem, recv_sem=yg_r.at[0],
            device_id=(g, f, part), device_id_type=MESH,
        ).wait_send()

    bar = pltpu.get_barrier_semaphore()

    def greet(dev):
        pl.semaphore_signal(bar, inc=1, device_id=dev, device_id_type=MESH)

    for tt in (part, right, left):
        greet((g, f, tt))
    loop(1, NF, lambda i: greet((g, (f + i) % NF, t)))
    loop(0, NZ, lambda i: greet((1 - g, i * NY + y, t)))

    gain[...] = jnp.broadcast_to(column(gain_t[...], 32), (32, 128))

    def cast(e):
        yy, z2 = e % NY, e // NY
        wg[yy, z2, 0:32, :] = (gain[...] * gate[e]).astype(BF)
        wg[yy, z2, 32:64, :] = (gain[...] * up[e]).astype(BF)
        wd[yy, z2] = down_t[e].astype(BF)

    loop(0, NF, cast)
    pl.semaphore_wait(bar, 3 + NF - 1 + NZ)

    def y_send(j, w, wy, ssem, rsems):
        yy = (y + ring_offset(j, NY)) % NY
        loop(0, NZ, lambda i: send(
            w.at[yy, i], wy.at[j - 1, i], ssem, rsems.at[j - 1], (g, z * NY + yy, t)))

    def z_send(jz, yy, block, s, wz, ssem, rsems):
        to = (zz + ring_offset(jz, NR)) % NR
        row = zz * NY + s
        send(block.at[to % NZ], wz.at[row], ssem, rsems.at[row],
             (to // NZ, (to % NZ) * NY + yy, t))

    loop(1, NY, lambda j: y_send(j, wg, wyg, snd.at[0], yg_r))
    loop(1, NR, lambda j: z_send(j, y, wg.at[y], y, zg, snd.at[1], zg_r))

    e_iota = lax.broadcasted_iota(jnp.int32, (NF, 256), 0)
    hit = (ids_t[0:1, :] == e_iota) | (ids_t[1:2, :] == e_iota)
    before = (
        lax.broadcasted_iota(jnp.int32, (256, 256), 0)
        < lax.broadcasted_iota(jnp.int32, (256, 256), 1)
    )
    rank = jnp.dot(hit.astype(F32).astype(BF), before.astype(F32).astype(BF),
                   preferred_element_type=F32)
    rt[...] = jnp.where(hit, rank, -1.0)
    r_iota = lax.broadcasted_iota(jnp.int32, (CAP, 256), 0).astype(F32)

    def slots(e):
        mask = rt[pl.ds(e, 1), :] == r_iota
        p0[e] = jnp.where(mask & (ids_t[0:1, :] == e), 1.0, 0.0).astype(BF)
        p1[e] = jnp.where(mask & (ids_t[1:2, :] == e), 1.0, 0.0).astype(BF)

    loop(0, NF, slots)
    floated = tok[...].astype(F32)
    inv = lax.rsqrt(jnp.mean(floated * floated, axis=-1, keepdims=True) + EPS)
    cols = pl.ds(pl.multiple_of(t * 256, 256), 256)
    normed = (tok[:, cols].astype(F32) * inv).astype(BF)

    def gather_rows(b):
        e = pl.ds(b * 8, 8)
        pick = (p0[e] + p1[e]).reshape(256, 256)
        rows = jnp.dot(pick, normed, preferred_element_type=F32)
        tsend[e] = rows.astype(BF).reshape(8, CAP, 256)

    loop(0, NZ, gather_rows)

    def t_send(i):
        e = ((z + i // NY) % NZ) * NY + (y + i % NY) % NY
        send(tsend.at[e], xin.at[t, f], snd.at[2], tk_r.at[f], (g, e, t))

    loop(1, NF, t_send)
    xin[t, f] = tsend[f]

    loop(1, NY, lambda j: y_send(j, wd, wyd, snd.at[8], yd_r))
    loop(1, NR, lambda j: z_send(j, y, wd.at[y], y, zd, snd.at[9], zd_r))
    zg[zz * NY + y] = wg[y, z]
    zd[zz * NY + y] = wd[y, z]

    def y_forward(j, wy, wz, ssem, rsems, yrsems):
        s = (y + NY - ring_offset(j, NY)) % NY
        arrived(wy.at[j - 1], yrsems.at[j - 1])
        loop(1, NR, lambda i: z_send(i, y, wy.at[j - 1], s, wz, ssem, rsems))
        wz[zz * NY + s] = wy[j - 1, z]

    loop(1, NY, lambda j: y_forward(j, wyg, zg, snd.at[1], zg_r, yg_r))

    def quarter(k):
        return (z + NZ - k) % NZ

    def pieces(tp, lo, n, kind, k, to):
        def one(i):
            blk = xin.at[tp, lo + i]
            send(blk, blk, snd.at[3], g_r.at[kind, k], (g, f, to))

        loop(0, n, one)

    def x_first(k):
        q = quarter(k)

        def one(i):
            s = q * NY + i

            @pl.when(s != f)
            def _():
                arrived(xin.at[t, s], tk_r.at[s])

            pieces(t, s, 1, 0, k, right)
            pieces(t, s, 1, 1, k, left)
            pieces(t, s, 1, 4, k, part)

        loop(0, NY, one)

    def x_second(k):
        q = quarter(k) * NY
        for side, kind, to, lo in ((left, 0, right, 0), (right, 1, left, 4)):
            arrived(xin.at[side, pl.ds(q, NY)], g_r.at[kind, k])
            pieces(side, q + lo, 4, kind + 2, k, to)
            pieces(side, q, NY, kind + 5, k, part)

    def x_third(k):
        q = quarter(k) * NY
        arrived(xin.at[opp, pl.ds(q, 4)], g_r.at[2, k])
        arrived(xin.at[opp, pl.ds(q + 4, 4)], g_r.at[3, k])
        pieces(opp, q, NY, 7, k, part)

    def x_step(k):
        @pl.when(k < NZ)
        def _():
            x_first(k)

        @pl.when((k >= 1) & (k < NZ + 1))
        def _():
            x_second(k - 1)

        @pl.when(k >= 2)
        def _():
            x_third(k - 2)

    loop(0, NZ + 2, x_step)
    loop(1, NY, lambda j: y_forward(j, wyd, zd, snd.at[9], zd_r, yd_r))
    flip = 1 - 2 * c

    def from_partner(k):
        q = pl.ds(quarter(k) * NY, NY)
        for side, kind in ((part, 4), (left + flip, 5), (right + flip, 6), (opp + flip, 7)):
            arrived(xin.at[side, q], g_r.at[kind, k])

    loop(0, NZ, from_partner)

    def w_arrived(i, wz, rsems):
        @pl.when(i // NY != zz)
        def _():
            arrived(wz.at[i], rsems.at[i])

    loop(0, 2 * NF, lambda i: w_arrived(i, zg, zg_r))

    def hidden(q):
        acc = jnp.zeros((256, 256), F32)
        for s in range(8):
            w = jnp.concatenate(
                [zg[8 * s:8 * s + 8, 0:32, :].reshape(256, 128),
                 zg[8 * s:8 * s + 8, 32:64, :].reshape(256, 128)], axis=1)
            acc += jnp.dot(xin[s, pl.ds(q * NY, NY)].reshape(256, 256), w,
                           preferred_element_type=F32)
        a, b = acc[:, 0:128], acc[:, 128:256]
        hid[pl.ds(2 * q, 2)] = (a / (1.0 + jnp.exp(-a)) * b).astype(BF).reshape(2, RB, 128)

    loop(0, NZ, hidden)
    loop(0, 2 * NF, lambda i: w_arrived(i, zd, zd_r))

    def which(k):
        return quarter(k // 2) * 2 + k % 2

    def layer(k):
        h = hid[which(k)]
        for j in range(NX):
            for cc in (1 - c, c):
                blk = ((x + j) % NX) * 2 + cc
                d = zd[pl.ds(blk * 8, 8)].reshape(256, 128)
                o = lax.dot_general(h, d, (((1,), (1,)), ((), ())), preferred_element_type=F32)
                if cc is c:
                    own[k, j] = o
                else:
                    psend[k, j] = o.astype(BF)
        send(psend.at[k], precv.at[k], snd.at[4], s_r.at[0, k], (g, f, part))

    LO, HI = pl.ds(0, RB // 2), pl.ds(RB // 2, RB // 2)

    def r_first(k):
        arrived(precv.at[k], s_r.at[0, k])
        sbuf[k, 1] = (own[k, 2] + precv[k, 2].astype(F32)).astype(BF)
        send(sbuf.at[k, 1, LO], r1.at[k, 0], snd.at[5], s_r.at[1, k], (g, f, right))
        send(sbuf.at[k, 1, HI], r1.at[k, 1], snd.at[5], s_r.at[2, k], (g, f, left))

    def r_second(k):
        for j, i, at, plain, to in ((1, 0, LO, HI, right), (3, 1, HI, LO, left)):
            arrived(r1.at[k, i], s_r.at[1 + i, k])
            sbuf[k, j - 1, at] = (
                own[k, j, at] + precv[k, j, at].astype(F32) + r1[k, i].astype(F32)
            ).astype(BF)
            sbuf[k, j - 1, plain] = (own[k, j, plain] + precv[k, j, plain].astype(F32)).astype(BF)
            send(sbuf.at[k, j - 1], r2.at[k, i], snd.at[6], s_r.at[3 + i, k], (g, f, to))

    def r_third(k):
        arrived(r2.at[k, 0], s_r.at[3, k])
        arrived(r2.at[k, 1], s_r.at[4, k])
        total = (own[k, 0] + precv[k, 0].astype(F32)) + r2[k, 0].astype(F32) + r2[k, 1].astype(F32)
        q = which(k)
        fin[q] = total.astype(BF).reshape(4, CAP, 256)

        def back(i):
            s = q * 4 + i

            @pl.when(s != f)
            def _():
                send(fin.at[q, i], ret.at[f], snd.at[7], ret_r.at[f], (g, s, t))

            @pl.when(s == f)
            def _():
                ret[s] = fin[q, i]

        loop(0, 4, back)

    def r_step(k):
        for lag, stage in ((0, layer), (1, r_first), (1 + LAG1, r_second), (1 + LAG1 + LAG2, r_third)):
            @pl.when((k >= lag) & (k < CH + lag))
            def _():
                stage(k - lag)

    loop(0, CH + 1 + LAG1 + LAG2, r_step)

    def store(i):
        gate_o[i] = zg[i, 0:32, :]
        up_o[i] = zg[i, 32:64, :]

    loop(0, 2 * NF, store)
    for j in range(16):
        blk = zd[4 * j:4 * j + 4].reshape(128, 128)
        down_o[:, 128 * j:128 * j + 128] = blk.astype(F32).T.astype(BF)
    s0, s1 = column(score_t[0:1, :], 256), column(score_t[1:2, :], 256)
    both = s0 + s1

    def back_arrived(i):
        @pl.when(i != f)
        def _():
            arrived(ret.at[i], ret_r.at[i])

    loop(0, NF, back_arrived)
    rows = ret[...].reshape(NF * CAP, 256)
    dims = (((0,), (0,)), ((), ()))
    a = lax.dot_general(p0[...].reshape(NF * CAP, 256), rows, dims, preferred_element_type=F32)
    b = lax.dot_general(p1[...].reshape(NF * CAP, 256), rows, dims, preferred_element_type=F32)
    mixed_o[...] = (a * (s0 / both) + b * (s1 / both)).astype(BF)

    nz = (NR - 1) * NY
    sent(wg.at[pl.ds(0, NY - 1)], snd.at[0])
    sent(zg.at[pl.ds(0, nz)], snd.at[1])
    sent(tsend.at[pl.ds(0, NF - 1)], snd.at[2])
    sent(xin.at[pl.ds(0, 7)], snd.at[3])
    sent(psend, snd.at[4])
    sent(r1, snd.at[5])
    sent(r2, snd.at[6])
    sent(ret.at[pl.ds(0, NF - 1)], snd.at[7])
    sent(wd.at[pl.ds(0, NY - 1)], snd.at[8])
    sent(zd.at[pl.ds(0, nz)], snd.at[9])


def write_out(gate_v, up_v, down_v, mixed_v, gate_o, up_o, down_o, mixed_o, sem):
    copies = [
        pltpu.make_async_copy(a, b, sem.at[i])
        for i, (a, b) in enumerate(
            ((gate_v, gate_o), (up_v, up_o), (down_v, down_o), (mixed_v, mixed_o)))
    ]
    for cp in copies:
        cp.start()
    for cp in copies:
        cp.wait()


def on_device(tokens, norm_gain, gate_train, up_train, down_train, expert_ids, route_score):
    vm = pl.BlockSpec(memory_space=pltpu.VMEM)
    hbm = pl.BlockSpec(memory_space=pl.ANY)
    dma = pltpu.SemaphoreType.DMA
    shapes = ((2 * NF, 32, 128), (2 * NF, 32, 128), (128, 2048), (256, 256))
    V = pltpu.VMEM
    held = pl.pallas_call(
        kernel,
        out_shape=tuple(V(s, BF) for s in shapes),
        in_specs=[vm] * 7,
        out_specs=(vm,) * 4,
        scratch_shapes=[
            V((32, 128), F32),
            V((NY, NZ, 64, 128), BF),
            V((NY, NZ, 32, 128), BF),
            V((NY - 1, NZ, 64, 128), BF),
            V((NY - 1, NZ, 32, 128), BF),
            V((2 * NF, 64, 128), BF),
            V((2 * NF, 32, 128), BF),
            V((NF, CAP, 256), BF),
            V((8, NF, CAP, 256), BF),
            V((NF, 256), F32),
            V((NF, CAP, 256), BF),
            V((NF, CAP, 256), BF),
            V((CH, RB, 128), BF),
            V((CH, NX, RB, 256), F32),
            V((CH, NX, RB, 256), BF),
            V((CH, NX, RB, 256), BF),
            V((CH, 3, RB, 256), BF),
            V((CH, 2, RB // 2, 256), BF),
            V((CH, 2, RB, 256), BF),
            V((CH, 4, CAP, 256), BF),
            V((NF, CAP, 256), BF),
            dma((NY - 1,)), dma((NY - 1,)), dma((2 * NF,)), dma((2 * NF,)), dma((NF,)),
            dma((8, NZ)), dma((5, CH)), dma((NF,)), dma((10,)),
        ],
        compiler_params=pltpu.CompilerParams(collective_id=0, has_side_effects=True),
    )(
        tokens, expert_ids.T, route_score.T, norm_gain[None, :], gate_train, up_train,
        down_train.transpose(0, 2, 1),
    )
    gate_r, up_r, down_r, mixed = pl.pallas_call(
        write_out,
        out_shape=tuple(jax.ShapeDtypeStruct(s, BF) for s in shapes),
        in_specs=[vm] * 4,
        out_specs=(hbm,) * 4,
        scratch_shapes=[dma((4,))],
    )(*[pltpu.with_memory_space_constraint(h, pltpu.VMEM) for h in held])
    return gate_r.reshape(1, 2048, 128), up_r.reshape(1, 2048, 128), down_r[None], mixed


def solution(mesh):
    return jax.shard_map(
        on_device,
        mesh=mesh,
        in_specs=(
            P(("gr", "fs"), None),
            P(("gr", "fs")),
            P(None, ("gr", "fs"), "tp"),
            P(None, ("gr", "fs"), "tp"),
            P(None, "tp", ("gr", "fs")),
            P(("gr", "fs"), None),
            P(("gr", "fs"), None),
        ),
        out_specs=(
            P("fs", None, "tp"),
            P("fs", None, "tp"),
            P("fs", "tp", None),
            P(("gr", "fs"), "tp"),
        ),
        check_vma=False,
    )
```

```python
import jax
import jax.numpy as jnp
from jax import lax
from jax.experimental import pallas as pl
from jax.experimental.pallas import tpu as pltpu
from jax.sharding import PartitionSpec as P

EPS = 1e-06
NY, NZ, NX = 8, 4, 4
NF = NY * NZ
NR = 2 * NZ
CAP = 32
CH = 8
RB, CQ = 1024 // CH, CH // NZ
LAG1, LAG2 = 3, 3
MESH = pl.DeviceIdType.MESH
BF, F32 = jnp.bfloat16, jnp.float32


OFFS = (1, 7, 2, 6, 3, 5, 4)


def rem(a, n):
    return lax.rem(a, jnp.int32(n))


def div(a, n):
    return lax.div(a, jnp.int32(n))


def loop(lo, hi, fn):
    def body(i, carry):
        fn(i)
        return carry

    lax.fori_loop(lo, hi, body, 0)


def column(row, n):
    eye = lax.broadcasted_iota(jnp.int32, (n, n), 0) == lax.broadcasted_iota(jnp.int32, (n, n), 1)
    return jnp.sum(jnp.where(eye, row, 0.0), axis=1, keepdims=True)


def kernel(
    tok_h, ids_t, score_t, gain_t, gate_h, up_h, down_h,
    gate_o, up_o, down_o, mixed_o,
    tok, gate, up, down_t, gain, wg, wd, wyg, wyd, zg, zd, tsend, xin, rt, p0, p1, hid,
    own, psend, precv, sbuf, r1, r2, fin, ret, acc,
    yg_r, yd_r, zg_r, zd_r, tk_r, g_r, s_r, ret_r, snd, in_sem, ready,
):
    g, f, t = lax.axis_index("gr"), lax.axis_index("fs"), lax.axis_index("tp")
    z, y, x, c = div(f, NY), rem(f, NY), div(t, 2), rem(t, 2)
    zz = g * NZ + z
    right, left = rem(x + 1, NX) * 2 + c, rem(x + 3, NX) * 2 + c
    opp, part = rem(x + 2, NX) * 2 + c, x * 2 + (1 - c)
    z_peer = [(div(q, NZ), rem(q, NZ)) for q in (rem(zz + o, NR) for o in OFFS)]

    def send(src, dst, ssem, rsem, dev):
        pltpu.make_async_remote_copy(
            src_ref=src, dst_ref=dst, send_sem=ssem, recv_sem=rsem,
            device_id=dev, device_id_type=MESH,
        ).start()

    def arrived(dst, rsem):
        pltpu.make_async_remote_copy(
            src_ref=dst, dst_ref=dst, send_sem=snd.at[0], recv_sem=rsem,
            device_id=(g, f, part), device_id_type=MESH,
        ).wait_recv()

    def sent(ref, ssem):
        pltpu.make_async_remote_copy(
            src_ref=ref, dst_ref=ref, send_sem=ssem, recv_sem=yg_r.at[0],
            device_id=(g, f, part), device_id_type=MESH,
        ).wait_send()

    loads = [
        pltpu.make_async_copy(a, b, in_sem.at[i])
        for i, (a, b) in enumerate(((gate_h, gate), (up_h, up), (down_h, down_t), (tok_h, tok)))
    ]
    for cp in loads:
        cp.start()

    bar = pltpu.get_barrier_semaphore()

    def greet(dev):
        pl.semaphore_signal(bar, inc=1, device_id=dev, device_id_type=MESH)

    for tt in (part, right, left):
        greet((g, f, tt))
    for o in OFFS:
        greet((g, z * NY + rem(y + o, NY), t))
    for g2, z2 in z_peer:
        greet((g2, z2 * NY + y, t))

    gain[...] = jnp.broadcast_to(column(gain_t[...], 32), (32, 128))

    def cast(yy):
        for z2 in range(NZ):
            e = z2 * NY + yy
            wg[yy, z2, 0:32, :] = (gain[...] * gate[e]).astype(BF)
            wg[yy, z2, 32:64, :] = (gain[...] * up[e]).astype(BF)

    def cast_down(yy):
        for z2 in range(NZ):
            wd[yy, z2] = down_t[z2 * NY + yy].astype(BF)

    loads[0].wait()
    loads[1].wait()
    loop(0, NY, cast)
    pl.semaphore_wait(bar, 3 + NY - 1 + NR - 1)
    loop(1, NZ, lambda i: pl.semaphore_signal(
        ready, inc=1, device_id=(g, rem(z + i, NZ) * NY + y, t), device_id_type=MESH))

    def y_sends(w, wy, ssem, rsems):
        for j, o in enumerate(OFFS):
            yy = rem(y + o, NY)
            for i in range(NZ):
                send(w.at[yy, i], wy.at[j, i], ssem, rsems.at[j], (g, z * NY + yy, t))

    def z_sends(block, s, wz, ssem, rsems):
        row = zz * NY + s
        for g2, z2 in z_peer:
            send(block.at[z2], wz.at[row], ssem, rsems.at[row], (g2, z2 * NY + y, t))
        wz[row] = block[z]

    y_sends(wg, wyg, snd.at[0], yg_r)
    z_sends(wg.at[y], y, zg, snd.at[1], zg_r)

    e_iota = lax.broadcasted_iota(jnp.int32, (NF, 256), 0)
    hit = (ids_t[0:1, :] == e_iota) | (ids_t[1:2, :] == e_iota)
    before = (
        lax.broadcasted_iota(jnp.int32, (256, 256), 0)
        < lax.broadcasted_iota(jnp.int32, (256, 256), 1)
    )
    rank = jnp.dot(hit.astype(F32).astype(BF), before.astype(F32).astype(BF),
                   preferred_element_type=F32)
    rt[...] = jnp.where(hit, rank, -1.0)
    r_iota = lax.broadcasted_iota(jnp.int32, (CAP, 256), 0).astype(F32)

    def slots(e):
        mask = rt[pl.ds(e, 1), :] == r_iota
        p0[e] = jnp.where(mask & (ids_t[0:1, :] == e), 1.0, 0.0).astype(BF)
        p1[e] = jnp.where(mask & (ids_t[1:2, :] == e), 1.0, 0.0).astype(BF)

    loop(0, NF, slots)
    loads[3].wait()
    floated = tok[...].astype(F32)
    inv = lax.rsqrt(jnp.mean(floated * floated, axis=-1, keepdims=True) + EPS)
    cols = pl.ds(pl.multiple_of(t * 256, 256), 256)
    normed = (tok[:, cols].astype(F32) * inv).astype(BF)

    def dispatch(k):
        q = rem(z + k, NZ)
        e = pl.ds(q * NY, NY)
        pick = (p0[e] + p1[e]).reshape(256, 256)
        rows = jnp.dot(pick, normed, preferred_element_type=F32)
        tsend[e] = rows.astype(BF).reshape(8, CAP, 256)
        for i in range(NY):
            to = q * NY + rem(y + i, NY)
            if i:
                send(tsend.at[to], xin.at[t, f], snd.at[2], tk_r.at[f], (g, to, t))
            else:
                @pl.when(to != f)
                def _():
                    send(tsend.at[to], xin.at[t, f], snd.at[2], tk_r.at[f], (g, to, t))

    pl.semaphore_wait(ready, NZ - 1)
    loop(0, NZ, dispatch)
    xin[t, f] = tsend[f]

    loads[2].wait()
    loop(0, NY, cast_down)
    y_sends(wd, wyd, snd.at[8], yd_r)
    z_sends(wd.at[y], y, zd, snd.at[9], zd_r)

    def y_forward(j, wy, wz, ssem, rsems, yrsems):
        s = rem(y + NY - OFFS[j], NY)
        arrived(wy.at[j], yrsems.at[j])
        z_sends(wy.at[j], s, wz, ssem, rsems)

    for j in range(NY - 1):
        y_forward(j, wyg, zg, snd.at[1], zg_r, yg_r)

    def quarter(k):
        return rem(z + NZ - k, NZ)

    def pieces(tp, lo, n, kind, k, to):
        def one(i):
            blk = xin.at[tp, lo + i]
            send(blk, blk, snd.at[3], g_r.at[kind, k], (g, f, to))

        loop(0, n, one)

    def x_first(k):
        q = quarter(k)

        def one(i):
            s = q * NY + i

            @pl.when(s != f)
            def _():
                arrived(xin.at[t, s], tk_r.at[s])

            pieces(t, s, 1, 0, k, right)
            pieces(t, s, 1, 1, k, left)
            pieces(t, s, 1, 4, k, part)

        loop(0, NY, one)

    def x_second(k):
        q = quarter(k) * NY
        for side, kind, to, lo in ((left, 0, right, 0), (right, 1, left, 4)):
            arrived(xin.at[side, pl.ds(q, NY)], g_r.at[kind, k])
            pieces(side, q + lo, 4, kind + 2, k, to)
            pieces(side, q, NY, kind + 5, k, part)

    def x_third(k):
        q = quarter(k) * NY
        arrived(xin.at[opp, pl.ds(q, 4)], g_r.at[2, k])
        arrived(xin.at[opp, pl.ds(q + 4, 4)], g_r.at[3, k])
        pieces(opp, q, NY, 7, k, part)

    def x_step(k):
        @pl.when(k < NZ)
        def _():
            x_first(k)

        @pl.when((k >= 1) & (k < NZ + 1))
        def _():
            x_second(k - 1)

        @pl.when(k >= 2)
        def _():
            x_third(k - 2)

    loop(0, NZ + 2, x_step)
    for j in range(NY - 1):
        y_forward(j, wyd, zd, snd.at[9], zd_r, yd_r)
    flip = 1 - 2 * c

    def from_partner(k):
        q = pl.ds(quarter(k) * NY, NY)
        for side, kind in ((part, 4), (left + flip, 5), (right + flip, 6), (opp + flip, 7)):
            arrived(xin.at[side, q], g_r.at[kind, k])

    loop(0, NZ, from_partner)

    def w_arrived(i, wz, rsems):
        @pl.when(div(i, NY) != zz)
        def _():
            arrived(wz.at[i], rsems.at[i])

    loop(0, 2 * NF, lambda i: w_arrived(i, zg, zg_r))

    def hidden(q):
        acc = jnp.zeros((256, 256), F32)
        for s in range(8):
            w = jnp.concatenate(
                [zg[8 * s:8 * s + 8, 0:32, :].reshape(256, 128),
                 zg[8 * s:8 * s + 8, 32:64, :].reshape(256, 128)], axis=1)
            acc += jnp.dot(xin[s, pl.ds(q * NY, NY)].reshape(256, 256), w,
                           preferred_element_type=F32)
        a, b = acc[:, 0:128], acc[:, 128:256]
        hid[pl.ds(CQ * q, CQ)] = (a / (1.0 + jnp.exp(-a)) * b).astype(BF).reshape(CQ, RB, 128)

    loop(0, NZ, hidden)
    loop(0, 2 * NF, lambda i: w_arrived(i, zd, zd_r))

    def which(k):
        return rem(z + 1 + div(k, CQ), NZ) * CQ + rem(k, CQ)

    def layer(k):
        h = hid[which(k)]
        for j in range(NX):
            for cc in (1 - c, c):
                blk = rem(x + j, NX) * 2 + cc
                d = zd[pl.ds(blk * 8, 8)].reshape(256, 128)
                o = lax.dot_general(h, d, (((1,), (1,)), ((), ())), preferred_element_type=F32)
                if cc is c:
                    own[k, j] = o
                else:
                    psend[k, j] = o.astype(BF)
        send(psend.at[k], precv.at[k], snd.at[4], s_r.at[0, k], (g, f, part))

    LO, HI = pl.ds(0, RB // 2), pl.ds(RB // 2, RB // 2)

    def r_first(k):
        arrived(precv.at[k], s_r.at[0, k])
        sbuf[k, 1] = (own[k, 2] + precv[k, 2].astype(F32)).astype(BF)
        send(sbuf.at[k, 1, LO], r1.at[k, 0], snd.at[5], s_r.at[1, k], (g, f, right))
        send(sbuf.at[k, 1, HI], r1.at[k, 1], snd.at[5], s_r.at[2, k], (g, f, left))

    def r_second(k):
        for j, i, at, plain, to in ((1, 0, LO, HI, right), (3, 1, HI, LO, left)):
            arrived(r1.at[k, i], s_r.at[1 + i, k])
            sbuf[k, j - 1, at] = (
                own[k, j, at] + precv[k, j, at].astype(F32) + r1[k, i].astype(F32)
            ).astype(BF)
            sbuf[k, j - 1, plain] = (own[k, j, plain] + precv[k, j, plain].astype(F32)).astype(BF)
            send(sbuf.at[k, j - 1], r2.at[k, i], snd.at[6], s_r.at[3 + i, k], (g, f, to))

    def r_third(k):
        arrived(r2.at[k, 0], s_r.at[3, k])
        arrived(r2.at[k, 1], s_r.at[4, k])
        total = (own[k, 0] + precv[k, 0].astype(F32)) + r2[k, 0].astype(F32) + r2[k, 1].astype(F32)
        q = which(k)
        fin[q] = total.astype(BF).reshape(NY // CQ, CAP, 256)

        def back(i):
            s = q * (NY // CQ) + i

            @pl.when(s != f)
            def _():
                send(fin.at[q, i], ret.at[f], snd.at[7], ret_r.at[f], (g, s, t))

            @pl.when(s == f)
            def _():
                ret[s] = fin[q, i]

        loop(0, NY // CQ, back)

    def r_step(k):
        for lag, stage in ((0, layer), (1, r_first), (1 + LAG1, r_second), (1 + LAG1 + LAG2, r_third)):
            @pl.when((k >= lag) & (k < CH + lag))
            def _():
                stage(k - lag)

    loop(0, CH + 1 + LAG1 + LAG2, r_step)

    def store(i):
        gate_o[i] = zg[i, 0:32, :]
        up_o[i] = zg[i, 32:64, :]

    loop(0, 2 * NF, store)
    for j in range(16):
        blk = zd[4 * j:4 * j + 4].reshape(128, 128)
        down_o[:, 128 * j:128 * j + 128] = blk.astype(F32).T.astype(BF)
    s0, s1 = column(score_t[0:1, :], 256), column(score_t[1:2, :], 256)
    both = s0 + s1

    acc[...] = jnp.zeros_like(acc)

    def combine(k):
        q = rem(z + NZ - 1 - k, NZ)

        def back_arrived(i):
            @pl.when(q * NY + i != f)
            def _():
                arrived(ret.at[q * NY + i], ret_r.at[q * NY + i])

        loop(0, NY, back_arrived)
        e = pl.ds(q * NY, NY)
        rows = ret[e].reshape(256, 256)
        for i, p in enumerate((p0, p1)):
            acc[i] += lax.dot_general(p[e].reshape(256, 256), rows, (((0,), (0,)), ((), ())),
                                      preferred_element_type=F32)

    loop(0, NZ, combine)
    mixed_o[...] = (acc[0] * (s0 / both) + acc[1] * (s1 / both)).astype(BF)

    nz = (NR - 1) * NY
    sent(wg.at[pl.ds(0, NY - 1)], snd.at[0])
    sent(zg.at[pl.ds(0, nz)], snd.at[1])
    sent(tsend.at[pl.ds(0, NF - 1)], snd.at[2])
    sent(xin.at[pl.ds(0, 7)], snd.at[3])
    sent(psend, snd.at[4])
    sent(r1, snd.at[5])
    sent(r2, snd.at[6])
    sent(ret.at[pl.ds(0, NF - 1)], snd.at[7])
    sent(wd.at[pl.ds(0, NY - 1)], snd.at[8])
    sent(zd.at[pl.ds(0, nz)], snd.at[9])


def write_out(gate_v, up_v, down_v, mixed_v, gate_o, up_o, down_o, mixed_o, sem):
    copies = [
        pltpu.make_async_copy(a, b, sem.at[i])
        for i, (a, b) in enumerate(
            ((gate_v, gate_o), (up_v, up_o), (down_v, down_o), (mixed_v, mixed_o)))
    ]
    for cp in copies:
        cp.start()
    for cp in copies:
        cp.wait()


def on_device(tokens, norm_gain, gate_train, up_train, down_train, expert_ids, route_score):
    vm = pl.BlockSpec(memory_space=pltpu.VMEM)
    hbm = pl.BlockSpec(memory_space=pl.ANY)
    dma = pltpu.SemaphoreType.DMA
    shapes = ((2 * NF, 32, 128), (2 * NF, 32, 128), (128, 2048), (256, 256))
    V = pltpu.VMEM
    held = pl.pallas_call(
        kernel,
        out_shape=tuple(V(s, BF) for s in shapes),
        in_specs=[hbm, vm, vm, vm, hbm, hbm, hbm],
        out_specs=(vm,) * 4,
        scratch_shapes=[
            V((256, 2048), BF), V((NF, 32, 128), F32), V((NF, 32, 128), F32), V((NF, 32, 128), F32),
            V((32, 128), F32),
            V((NY, NZ, 64, 128), BF),
            V((NY, NZ, 32, 128), BF),
            V((NY - 1, NZ, 64, 128), BF),
            V((NY - 1, NZ, 32, 128), BF),
            V((2 * NF, 64, 128), BF),
            V((2 * NF, 32, 128), BF),
            V((NF, CAP, 256), BF),
            V((8, NF, CAP, 256), BF),
            V((NF, 256), F32),
            V((NF, CAP, 256), BF),
            V((NF, CAP, 256), BF),
            V((CH, RB, 128), BF),
            V((CH, NX, RB, 256), F32),
            V((CH, NX, RB, 256), BF),
            V((CH, NX, RB, 256), BF),
            V((CH, 3, RB, 256), BF),
            V((CH, 2, RB // 2, 256), BF),
            V((CH, 2, RB, 256), BF),
            V((CH, NY // CQ, CAP, 256), BF),
            V((NF, CAP, 256), BF),
            V((2, 256, 256), F32),
            dma((NY - 1,)), dma((NY - 1,)), dma((2 * NF,)), dma((2 * NF,)), dma((NF,)),
            dma((8, NZ)), dma((5, CH)), dma((NF,)), dma((10,)), dma((4,)),
            pltpu.SemaphoreType.REGULAR,
        ],
        compiler_params=pltpu.CompilerParams(collective_id=0, has_side_effects=True),
    )(
        tokens, expert_ids.T, route_score.T, norm_gain[None, :], gate_train, up_train,
        down_train.transpose(0, 2, 1),
    )
    gate_r, up_r, down_r, mixed = pl.pallas_call(
        write_out,
        out_shape=tuple(jax.ShapeDtypeStruct(s, BF) for s in shapes),
        in_specs=[vm] * 4,
        out_specs=(hbm,) * 4,
        scratch_shapes=[dma((4,))],
    )(*[pltpu.with_memory_space_constraint(h, pltpu.VMEM) for h in held])
    return gate_r.reshape(1, 2048, 128), up_r.reshape(1, 2048, 128), down_r[None], mixed


def solution(mesh):
    return jax.shard_map(
        on_device,
        mesh=mesh,
        in_specs=(
            P(("gr", "fs"), None),
            P(("gr", "fs")),
            P(None, ("gr", "fs"), "tp"),
            P(None, ("gr", "fs"), "tp"),
            P(None, "tp", ("gr", "fs")),
            P(("gr", "fs"), None),
            P(("gr", "fs"), None),
        ),
        out_specs=(
            P("fs", None, "tp"),
            P("fs", None, "tp"),
            P("fs", "tp", None),
            P(("gr", "fs"), "tp"),
        ),
        check_vma=False,
    )
```

```python
import jax
import jax.numpy as jnp
from jax import lax
from jax.experimental import pallas as pl
from jax.experimental.pallas import tpu as pltpu
from jax.sharding import PartitionSpec as P

EPS = 1e-06
NY, NZ, NX = 8, 4, 4
NF = NY * NZ
NR = 2 * NZ
CAP = 32
CH = 8
RB, CQ = 1024 // CH, CH // NZ
LAG1, LAG2 = 3, 3
MESH = pl.DeviceIdType.MESH
BF, F32 = jnp.bfloat16, jnp.float32


OFFS = (1, 7, 2, 6, 3, 5, 4)


def rem(a, n):
    return lax.rem(a, jnp.int32(n))


def div(a, n):
    return lax.div(a, jnp.int32(n))


def loop(lo, hi, fn):
    def body(i, carry):
        fn(i)
        return carry

    lax.fori_loop(lo, hi, body, 0)


def column(row, n):
    eye = lax.broadcasted_iota(jnp.int32, (n, n), 0) == lax.broadcasted_iota(jnp.int32, (n, n), 1)
    return jnp.sum(jnp.where(eye, row, 0.0), axis=1, keepdims=True)


def kernel(
    tok_h, ids_t, score_t, gain_t, gate_h, up_h, down_h,
    gate_o, up_o, down_o, mixed_o,
    tok, gate, up, down_t, gain, wg, wd, wyg, wyd, zg, zd, tsend, xin, rt, p0, p1, hid,
    own, psend, precv, sbuf, r1, r2, fin, ret, acc,
    yg_r, yd_r, zg_r, zd_r, tk_r, g_r, s_r, ret_r, snd, in_sem, ready,
):
    g, f, t = lax.axis_index("gr"), lax.axis_index("fs"), lax.axis_index("tp")
    z, y, x, c = div(f, NY), rem(f, NY), div(t, 2), rem(t, 2)
    zz = g * NZ + z
    right, left = rem(x + 1, NX) * 2 + c, rem(x + 3, NX) * 2 + c
    opp, part = rem(x + 2, NX) * 2 + c, x * 2 + (1 - c)
    z_peer = [(div(q, NZ), rem(q, NZ)) for q in (rem(zz + o, NR) for o in OFFS)]

    def send(src, dst, ssem, rsem, dev):
        pltpu.make_async_remote_copy(
            src_ref=src, dst_ref=dst, send_sem=ssem, recv_sem=rsem,
            device_id=dev, device_id_type=MESH,
        ).start()

    def arrived(dst, rsem):
        pltpu.make_async_remote_copy(
            src_ref=dst, dst_ref=dst, send_sem=snd.at[0], recv_sem=rsem,
            device_id=(g, f, part), device_id_type=MESH,
        ).wait_recv()

    def sent(ref, ssem):
        pltpu.make_async_remote_copy(
            src_ref=ref, dst_ref=ref, send_sem=ssem, recv_sem=yg_r.at[0],
            device_id=(g, f, part), device_id_type=MESH,
        ).wait_send()

    loads = [
        pltpu.make_async_copy(a, b, in_sem.at[i])
        for i, (a, b) in enumerate(((gate_h, gate), (up_h, up), (down_h, down_t), (tok_h, tok)))
    ]
    for cp in loads:
        cp.start()

    bar = pltpu.get_barrier_semaphore()

    def greet(dev):
        pl.semaphore_signal(bar, inc=1, device_id=dev, device_id_type=MESH)

    for tt in (part, right, left):
        greet((g, f, tt))
    for o in OFFS:
        greet((g, z * NY + rem(y + o, NY), t))
    for g2, z2 in z_peer:
        greet((g2, z2 * NY + y, t))

    gain[...] = jnp.broadcast_to(column(gain_t[...], 32), (32, 128))

    def cast(yy):
        for z2 in range(NZ):
            e = z2 * NY + yy
            wg[yy, z2, 0:32, :] = (gain[...] * gate[e]).astype(BF)
            wg[yy, z2, 32:64, :] = (gain[...] * up[e]).astype(BF)

    def cast_down(yy):
        for z2 in range(NZ):
            wd[yy, z2] = down_t[z2 * NY + yy].astype(BF)

    loads[0].wait()
    loads[1].wait()
    loop(0, NY, cast)
    pl.semaphore_wait(bar, 3 + NY - 1 + NR - 1)
    loop(1, NZ, lambda i: pl.semaphore_signal(
        ready, inc=1, device_id=(g, rem(z + i, NZ) * NY + y, t), device_id_type=MESH))

    def y_sends(w, wy, ssem, rsems):
        for j, o in enumerate(OFFS):
            yy = rem(y + o, NY)
            for i in range(NZ):
                send(w.at[yy, i], wy.at[j, i], ssem, rsems.at[j], (g, z * NY + yy, t))

    def z_sends(block, s, wz, ssem, rsems):
        row = zz * NY + s
        for g2, z2 in z_peer:
            send(block.at[z2], wz.at[row], ssem, rsems.at[row], (g2, z2 * NY + y, t))
        wz[row] = block[z]

    y_sends(wg, wyg, snd.at[0], yg_r)
    z_sends(wg.at[y], y, zg, snd.at[1], zg_r)

    e_iota = lax.broadcasted_iota(jnp.int32, (NF, 256), 0)
    hit = (ids_t[0:1, :] == e_iota) | (ids_t[1:2, :] == e_iota)
    before = (
        lax.broadcasted_iota(jnp.int32, (256, 256), 0)
        < lax.broadcasted_iota(jnp.int32, (256, 256), 1)
    )
    rank = jnp.dot(hit.astype(F32).astype(BF), before.astype(F32).astype(BF),
                   preferred_element_type=F32)
    rt[...] = jnp.where(hit, rank, -1.0)
    r_iota = lax.broadcasted_iota(jnp.int32, (CAP, 256), 0).astype(F32)

    def slots(e):
        mask = rt[pl.ds(e, 1), :] == r_iota
        p0[e] = jnp.where(mask & (ids_t[0:1, :] == e), 1.0, 0.0).astype(BF)
        p1[e] = jnp.where(mask & (ids_t[1:2, :] == e), 1.0, 0.0).astype(BF)

    loop(0, NF, slots)
    loads[3].wait()
    floated = tok[...].astype(F32)
    inv = lax.rsqrt(jnp.mean(floated * floated, axis=-1, keepdims=True) + EPS)
    cols = pl.ds(pl.multiple_of(t * 256, 256), 256)
    normed = (tok[:, cols].astype(F32) * inv).astype(BF)

    def dispatch(k):
        q = rem(z + k, NZ)
        e = pl.ds(q * NY, NY)
        pick = (p0[e] + p1[e]).reshape(256, 256)
        rows = jnp.dot(pick, normed, preferred_element_type=F32)
        tsend[e] = rows.astype(BF).reshape(8, CAP, 256)
        for i in range(NY):
            to = q * NY + rem(y + i, NY)
            if i:
                send(tsend.at[to], xin.at[t, f], snd.at[2], tk_r.at[f], (g, to, t))
            else:
                @pl.when(to != f)
                def _():
                    send(tsend.at[to], xin.at[t, f], snd.at[2], tk_r.at[f], (g, to, t))

    pl.semaphore_wait(ready, NZ - 1)
    loop(0, NZ, dispatch)
    xin[t, f] = tsend[f]

    loads[2].wait()
    loop(0, NY, cast_down)
    y_sends(wd, wyd, snd.at[8], yd_r)
    z_sends(wd.at[y], y, zd, snd.at[9], zd_r)

    def y_forward(j, wy, wz, ssem, rsems, yrsems):
        s = rem(y + NY - OFFS[j], NY)
        arrived(wy.at[j], yrsems.at[j])
        z_sends(wy.at[j], s, wz, ssem, rsems)


    def quarter(k):
        return rem(z + NZ - k, NZ)

    def pieces(tp, lo, n, kind, k, to):
        def one(i):
            blk = xin.at[tp, lo + i]
            send(blk, blk, snd.at[3], g_r.at[kind, k], (g, f, to))

        loop(0, n, one)

    def x_first(k):
        q = quarter(k)

        def one(i):
            s = q * NY + i

            @pl.when(s != f)
            def _():
                arrived(xin.at[t, s], tk_r.at[s])

            pieces(t, s, 1, 0, k, right)
            pieces(t, s, 1, 1, k, left)
            pieces(t, s, 1, 4, k, part)

        loop(0, NY, one)

    def x_second(k):
        q = quarter(k) * NY
        for side, kind, to, lo in ((left, 0, right, 0), (right, 1, left, 4)):
            arrived(xin.at[side, pl.ds(q, NY)], g_r.at[kind, k])
            pieces(side, q + lo, 4, kind + 2, k, to)
            pieces(side, q, NY, kind + 5, k, part)

    def x_third(k):
        q = quarter(k) * NY
        arrived(xin.at[opp, pl.ds(q, 4)], g_r.at[2, k])
        arrived(xin.at[opp, pl.ds(q + 4, 4)], g_r.at[3, k])
        pieces(opp, q, NY, 7, k, part)

    def x_step(k):
        @pl.when(k < NZ)
        def _():
            x_first(k)

        @pl.when(k == 3)
        def _():
            for j in range(NY - 1):
                y_forward(j, wyd, zd, snd.at[9], zd_r, yd_r)

        @pl.when((k >= 1) & (k < NZ + 1))
        def _():
            x_second(k - 1)

        @pl.when(k >= 2)
        def _():
            x_third(k - 2)

    for j in range(0, 4):
        y_forward(j, wyg, zg, snd.at[1], zg_r, yg_r)
    x_step(jnp.int32(0))
    for j in range(4, 7):
        y_forward(j, wyg, zg, snd.at[1], zg_r, yg_r)
    loop(1, NZ + 2, x_step)
    flip = 1 - 2 * c

    def from_partner(k):
        q = pl.ds(quarter(k) * NY, NY)
        for side, kind in ((part, 4), (left + flip, 5), (right + flip, 6), (opp + flip, 7)):
            arrived(xin.at[side, q], g_r.at[kind, k])

    loop(0, NZ, from_partner)

    def w_arrived(i, wz, rsems):
        @pl.when(div(i, NY) != zz)
        def _():
            arrived(wz.at[i], rsems.at[i])

    loop(0, 2 * NF, lambda i: w_arrived(i, zg, zg_r))

    def hidden(q):
        acc = jnp.zeros((256, 256), F32)
        for s in range(8):
            w = jnp.concatenate(
                [zg[8 * s:8 * s + 8, 0:32, :].reshape(256, 128),
                 zg[8 * s:8 * s + 8, 32:64, :].reshape(256, 128)], axis=1)
            acc += jnp.dot(xin[s, pl.ds(q * NY, NY)].reshape(256, 256), w,
                           preferred_element_type=F32)
        a, b = acc[:, 0:128], acc[:, 128:256]
        hid[pl.ds(CQ * q, CQ)] = (a / (1.0 + jnp.exp(-a)) * b).astype(BF).reshape(CQ, RB, 128)

    loop(0, NZ, hidden)
    loop(0, 2 * NF, lambda i: w_arrived(i, zd, zd_r))

    def which(k):
        return rem(z + 1 + div(k, CQ), NZ) * CQ + rem(k, CQ)

    def layer(k):
        h = hid[which(k)]
        for j in range(NX):
            for cc in (1 - c, c):
                blk = rem(x + j, NX) * 2 + cc
                d = zd[pl.ds(blk * 8, 8)].reshape(256, 128)
                o = lax.dot_general(h, d, (((1,), (1,)), ((), ())), preferred_element_type=F32)
                if cc is c:
                    own[k, j] = o
                else:
                    psend[k, j] = o.astype(BF)
        send(psend.at[k], precv.at[k], snd.at[4], s_r.at[0, k], (g, f, part))

    LO, HI = pl.ds(0, RB // 2), pl.ds(RB // 2, RB // 2)

    def r_first(k):
        arrived(precv.at[k], s_r.at[0, k])
        sbuf[k, 1] = (own[k, 2] + precv[k, 2].astype(F32)).astype(BF)
        send(sbuf.at[k, 1, LO], r1.at[k, 0], snd.at[5], s_r.at[1, k], (g, f, right))
        send(sbuf.at[k, 1, HI], r1.at[k, 1], snd.at[5], s_r.at[2, k], (g, f, left))

    def r_second(k):
        for j, i, at, plain, to in ((1, 0, LO, HI, right), (3, 1, HI, LO, left)):
            arrived(r1.at[k, i], s_r.at[1 + i, k])
            sbuf[k, j - 1, at] = (
                own[k, j, at] + precv[k, j, at].astype(F32) + r1[k, i].astype(F32)
            ).astype(BF)
            sbuf[k, j - 1, plain] = (own[k, j, plain] + precv[k, j, plain].astype(F32)).astype(BF)
            send(sbuf.at[k, j - 1], r2.at[k, i], snd.at[6], s_r.at[3 + i, k], (g, f, to))

    def r_third(k):
        arrived(r2.at[k, 0], s_r.at[3, k])
        arrived(r2.at[k, 1], s_r.at[4, k])
        total = (own[k, 0] + precv[k, 0].astype(F32)) + r2[k, 0].astype(F32) + r2[k, 1].astype(F32)
        q = which(k)
        fin[q] = total.astype(BF).reshape(NY // CQ, CAP, 256)

        def back(i):
            s = q * (NY // CQ) + i

            @pl.when(s != f)
            def _():
                send(fin.at[q, i], ret.at[f], snd.at[7], ret_r.at[f], (g, s, t))

            @pl.when(s == f)
            def _():
                ret[s] = fin[q, i]

        loop(0, NY // CQ, back)

    def r_step(k):
        for lag, stage in ((0, layer), (1, r_first), (1 + LAG1, r_second), (1 + LAG1 + LAG2, r_third)):
            @pl.when((k >= lag) & (k < CH + lag))
            def _():
                stage(k - lag)

    loop(0, CH + 1 + LAG1 + LAG2, r_step)

    def store(i):
        gate_o[i] = zg[i, 0:32, :]
        up_o[i] = zg[i, 32:64, :]

    loop(0, 2 * NF, store)
    for j in range(16):
        blk = zd[4 * j:4 * j + 4].reshape(128, 128)
        down_o[:, 128 * j:128 * j + 128] = blk.astype(F32).T.astype(BF)
    s0, s1 = column(score_t[0:1, :], 256), column(score_t[1:2, :], 256)
    both = s0 + s1

    acc[...] = jnp.zeros_like(acc)

    def combine(k):
        q = rem(z + NZ - 1 - k, NZ)

        def back_arrived(i):
            @pl.when(q * NY + i != f)
            def _():
                arrived(ret.at[q * NY + i], ret_r.at[q * NY + i])

        loop(0, NY, back_arrived)
        e = pl.ds(q * NY, NY)
        rows = ret[e].reshape(256, 256)
        for i, p in enumerate((p0, p1)):
            acc[i] += lax.dot_general(p[e].reshape(256, 256), rows, (((0,), (0,)), ((), ())),
                                      preferred_element_type=F32)

    loop(0, NZ, combine)
    mixed_o[...] = (acc[0] * (s0 / both) + acc[1] * (s1 / both)).astype(BF)

    nz = (NR - 1) * NY
    sent(wg.at[pl.ds(0, NY - 1)], snd.at[0])
    sent(zg.at[pl.ds(0, nz)], snd.at[1])
    sent(tsend.at[pl.ds(0, NF - 1)], snd.at[2])
    sent(xin.at[pl.ds(0, 7)], snd.at[3])
    sent(psend, snd.at[4])
    sent(r1, snd.at[5])
    sent(r2, snd.at[6])
    sent(ret.at[pl.ds(0, NF - 1)], snd.at[7])
    sent(wd.at[pl.ds(0, NY - 1)], snd.at[8])
    sent(zd.at[pl.ds(0, nz)], snd.at[9])


def write_out(gate_v, up_v, down_v, mixed_v, gate_o, up_o, down_o, mixed_o, sem):
    copies = [
        pltpu.make_async_copy(a, b, sem.at[i])
        for i, (a, b) in enumerate(
            ((gate_v, gate_o), (up_v, up_o), (down_v, down_o), (mixed_v, mixed_o)))
    ]
    for cp in copies:
        cp.start()
    for cp in copies:
        cp.wait()


def on_device(tokens, norm_gain, gate_train, up_train, down_train, expert_ids, route_score):
    vm = pl.BlockSpec(memory_space=pltpu.VMEM)
    hbm = pl.BlockSpec(memory_space=pl.ANY)
    dma = pltpu.SemaphoreType.DMA
    shapes = ((2 * NF, 32, 128), (2 * NF, 32, 128), (128, 2048), (256, 256))
    V = pltpu.VMEM
    held = pl.pallas_call(
        kernel,
        out_shape=tuple(V(s, BF) for s in shapes),
        in_specs=[hbm, vm, vm, vm, hbm, hbm, hbm],
        out_specs=(vm,) * 4,
        scratch_shapes=[
            V((256, 2048), BF), V((NF, 32, 128), F32), V((NF, 32, 128), F32), V((NF, 32, 128), F32),
            V((32, 128), F32),
            V((NY, NZ, 64, 128), BF),
            V((NY, NZ, 32, 128), BF),
            V((NY - 1, NZ, 64, 128), BF),
            V((NY - 1, NZ, 32, 128), BF),
            V((2 * NF, 64, 128), BF),
            V((2 * NF, 32, 128), BF),
            V((NF, CAP, 256), BF),
            V((8, NF, CAP, 256), BF),
            V((NF, 256), F32),
            V((NF, CAP, 256), BF),
            V((NF, CAP, 256), BF),
            V((CH, RB, 128), BF),
            V((CH, NX, RB, 256), F32),
            V((CH, NX, RB, 256), BF),
            V((CH, NX, RB, 256), BF),
            V((CH, 3, RB, 256), BF),
            V((CH, 2, RB // 2, 256), BF),
            V((CH, 2, RB, 256), BF),
            V((CH, NY // CQ, CAP, 256), BF),
            V((NF, CAP, 256), BF),
            V((2, 256, 256), F32),
            dma((NY - 1,)), dma((NY - 1,)), dma((2 * NF,)), dma((2 * NF,)), dma((NF,)),
            dma((8, NZ)), dma((5, CH)), dma((NF,)), dma((10,)), dma((4,)),
            pltpu.SemaphoreType.REGULAR,
        ],
        compiler_params=pltpu.CompilerParams(collective_id=0, has_side_effects=True),
    )(
        tokens, expert_ids.T, route_score.T, norm_gain[None, :], gate_train, up_train,
        down_train.transpose(0, 2, 1),
    )
    gate_r, up_r, down_r, mixed = pl.pallas_call(
        write_out,
        out_shape=tuple(jax.ShapeDtypeStruct(s, BF) for s in shapes),
        in_specs=[vm] * 4,
        out_specs=(hbm,) * 4,
        scratch_shapes=[dma((4,))],
    )(*[pltpu.with_memory_space_constraint(h, pltpu.VMEM) for h in held])
    return gate_r.reshape(1, 2048, 128), up_r.reshape(1, 2048, 128), down_r[None], mixed


def solution(mesh):
    return jax.shard_map(
        on_device,
        mesh=mesh,
        in_specs=(
            P(("gr", "fs"), None),
            P(("gr", "fs")),
            P(None, ("gr", "fs"), "tp"),
            P(None, ("gr", "fs"), "tp"),
            P(None, "tp", ("gr", "fs")),
            P(("gr", "fs"), None),
            P(("gr", "fs"), None),
        ),
        out_specs=(
            P("fs", None, "tp"),
            P("fs", None, "tp"),
            P("fs", "tp", None),
            P(("gr", "fs"), "tp"),
        ),
        check_vma=False,
    )
```
